256 devices in a mesh: dp: 4 (over x), kv: 32 (over z, y), tp: 2 (over core).
Axes of the slice: x: 4, y: 4, z: 8, core: 2. Of those that a mesh axis runs over, the one named last changes fastest.
Arguments:
- tokens: bfloat16 [4, 16384, 2048], P('dp', 'kv'), may hold values from -6 to 6
- w_query: bfloat16 [2048, 1024], P(None, 'tp'), as said below
- w_key: bfloat16 [2048, 1024], P(None, 'tp'), as said below
- w_value: bfloat16 [2048, 1024], P(None, 'tp'), may hold values from -0.125 to 0.125
- w_out: bfloat16 [1024, 2048], P('tp'), may hold values from -0.1875 to 0.1875
- chosen: int32 [4, 256, 16], P('dp', 'kv'), may hold values from -1 to 255, as said below
Outputs:
- mixed: bfloat16 [4, 16384, 2048], P('dp', ('kv', 'tp'))
- log_sums: float32 [4, 16, 16384], P('dp', 'tp', 'kv')
The draws below stay inside these ranges and needn't reach their ends.
Inputs may be any that keep to these rules, and one draw needn't show every extreme that they name: `chosen`: write d = b // 8 and j = b % 8 for query block b. Row b lists b first, then min(15, j + 2 * d) distinct earlier blocks, then -1. Of the blocks that the query blocks of one index d of kv list, at most 2 lie in the positions of any one other index; the first query block of every index d >= 1 lists 2 blocks of index d - 1, and, where it exists, 2 blocks of the index half the sequence earlier. `w_query`: A weight matrix with entries up to about 4. `w_key`: A weight matrix of entries of order 2048 to the power -1/2.
All inputs are finite; a program needn't handle non-finite values.
Results may differ from the reference program's by a relative error of at most 0.0093.
Values may be sent and summed in bfloat16 or wider, within the bound.
No kernel may reach another device: no remote copies, remote signals or barrier semaphores. Data moves between devices by JAX's collectives and lax.ppermute only.
A program may use at most 192 MiB of HBM per device.

```python
import jax
import jax.numpy as jnp
from jax import lax

D = 2048
HEADS = 16
HEAD_DIM = 64
BLOCK = 64
NSEL = 16
SEQS = 4
LENGTH = 16384
NBLK = 256
KB_DEV = 8
CAP = 2
N_TP = 2


def paired_weights(key):
    base = jax.random.fold_in(key, 11)
    scale = D ** (-0.5)
    key_weight = jnp.clip(jax.random.normal(jax.random.fold_in(base, 1), (D, HEADS * HEAD_DIM), jnp.float32), -6.0, 6.0) * scale
    free_weight = jnp.clip(jax.random.normal(jax.random.fold_in(base, 2), (D, HEADS * HEAD_DIM), jnp.float32), -6.0, 6.0) * scale
    query_weight = free_weight
    return (query_weight, key_weight)


def draw_w_query(key, part):
    return paired_weights(key)[0].astype(jnp.bfloat16)


def draw_w_key(key, part):
    return paired_weights(key)[1].astype(jnp.bfloat16)


def one_sequence(key):
    blocks = jnp.arange(NBLK, dtype=jnp.int32)
    owners = blocks // KB_DEV
    within = blocks % KB_DEV
    devices = NBLK // KB_DEV
    pair_scores = jax.random.randint(jax.random.fold_in(key, 1), (devices, devices, KB_DEV), 0, 65536) * KB_DEV + jnp.arange(KB_DEV, dtype=jnp.int32)
    ranks = jnp.sum((pair_scores[..., None, :] > pair_scores[..., :, None]).astype(jnp.int32), axis=-1)
    allowed_pair = ranks < CAP
    query_dev = owners[:, None]
    key_dev = owners[None, :]
    own_earlier = (key_dev == query_dev) & (blocks[None, :] < blocks[:, None])
    allowed_here = allowed_pair[query_dev, key_dev, within[None, :]]
    foreign = (key_dev < query_dev) & allowed_here
    candidate = own_earlier | foreign
    popular = (jax.random.randint(jax.random.fold_in(key, 2), (NBLK,), 0, 6) == 0).astype(jnp.int32)
    base = jax.random.randint(jax.random.fold_in(key, 3), (NBLK, NBLK), 0, 1024) + 4096 * popular[None, :]
    forced = foreign & (within[:, None] == 0) & ((key_dev == query_dev - 1) | (key_dev == query_dev - devices // 2))
    base = base + 65536 * forced.astype(jnp.int32)
    final = jnp.where(candidate, base * NBLK + blocks[None, :], -1)
    top_values, top_index = lax.top_k(final, NSEL - 1)
    picks = jnp.where(top_values >= 0, top_index, -1)
    return jnp.concatenate([blocks[:, None], picks], axis=1).astype(jnp.int32)


def draw_chosen(key, part):
    seq_keys = jax.vmap(lambda index: jax.random.fold_in(key, index))(jnp.arange(SEQS, dtype=jnp.int32))
    return jax.vmap(one_sequence)(seq_keys)


def block_scale(stream_key, shape, pieces, least, top_value):
    def one(position, blocks):
        draws = jax.random.uniform(jax.random.fold_in(jax.random.fold_in(stream_key, 6), position), (blocks,), jnp.float32, least / len(pieces), top_value / len(pieces))
        return jnp.repeat(jnp.exp(draws), shape[position] // blocks).reshape((-1,) + (1,) * (len(shape) - position - 1))

    loudness = one(*pieces[0])
    for cut in pieces[1:]:
        loudness = loudness * one(*cut)
    return loudness


def scatter_about(stream_key, extent, scale, limit, cuts=(), kind=jnp.bfloat16):
    drawn = scale * jax.random.normal(stream_key, extent, jnp.float32)
    if cuts:
        drawn = drawn * block_scale(stream_key, extent, cuts, -0.22, 0.18)
    return jnp.clip(drawn, -limit, limit).astype(kind)


def setup_inputs(seed: int = 0) -> dict:
    splits = jax.random.split(jax.random.key(seed), 7)
    return {
        "tokens": scatter_about(splits[0], (SEQS, LENGTH, D), 1.0, 6.0, ((0, 4), (1, 32))),
        "w_query": draw_w_query(jax.random.fold_in(splits[6], 71), 0),
        "w_key": draw_w_key(jax.random.fold_in(splits[6], 71), 0),
        "w_value": scatter_about(splits[3], (D, HEADS * HEAD_DIM), D ** -0.5, 0.125, ((1, 2),)),
        "w_out": scatter_about(splits[4], (HEADS * HEAD_DIM, D), (HEADS * HEAD_DIM) ** -0.5, 0.1875, ((0, 2),)),
        "chosen": draw_chosen(jax.random.fold_in(splits[6], 71), 0),
    }


def attend_sequence(inputs, w_query, w_key, w_value, w_out, listed):
    queries = jnp.dot(inputs, w_query, preferred_element_type=jnp.float32).astype(jnp.bfloat16)
    keys_all = jnp.dot(inputs, w_key, preferred_element_type=jnp.float32).astype(jnp.bfloat16)
    values_all = jnp.dot(inputs, w_value, preferred_element_type=jnp.float32).astype(jnp.bfloat16)
    width = queries.shape[1]
    query_blocks = queries.reshape(NBLK, BLOCK, HEADS, HEAD_DIM)
    key_blocks = keys_all.reshape(NBLK, BLOCK, HEADS, HEAD_DIM)
    value_blocks = values_all.reshape(NBLK, BLOCK, HEADS, HEAD_DIM)
    offsets = jnp.arange(BLOCK, dtype=jnp.int32)

    def one_block(args):
        query_block, row, index = args
        valid = row >= 0
        safe = jnp.where(valid, row, 0).astype(jnp.int32)
        keys_sel = key_blocks[safe].astype(jnp.float32)
        values_sel = value_blocks[safe].astype(jnp.float32)
        scores = jnp.einsum('qhd,skhd->hqsk', query_block.astype(jnp.float32), keys_sel) * (HEAD_DIM ** -0.5)
        key_pos = row[:, None] * BLOCK + offsets[None, :]
        query_pos = index * BLOCK + offsets
        allowed = valid[None, :, None] & (key_pos[None, :, :] <= query_pos[:, None, None])
        scores = jnp.where(allowed[None], scores, -jnp.inf)
        row_max = jnp.max(scores, axis=(2, 3), keepdims=True)
        exp_terms = jnp.exp(scores - row_max)
        row_sum = jnp.sum(exp_terms, axis=(2, 3), keepdims=True)
        weights = (exp_terms / row_sum).astype(jnp.bfloat16)
        attended = jnp.einsum('hqsk,skhd->qhd', weights.astype(jnp.float32), values_sel).astype(jnp.bfloat16)
        return attended.reshape(BLOCK, width), (row_max + jnp.log(row_sum))[:, :, 0, 0]

    attended, log_sums = lax.map(one_block, (query_blocks, listed, jnp.arange(NBLK, dtype=jnp.int32)))
    attended = attended.reshape(LENGTH, width)
    log_sums = jnp.transpose(log_sums, (1, 0, 2)).reshape(HEADS, LENGTH)
    share = width // N_TP
    total = jnp.zeros((LENGTH, w_out.shape[1]), jnp.float32)
    for shard in range(N_TP):
        partial_value = jnp.dot(attended[:, shard * share:(shard + 1) * share], w_out[shard * share:(shard + 1) * share],
                          preferred_element_type=jnp.float32).astype(jnp.bfloat16)
        total = total + partial_value.astype(jnp.float32)
    return total.astype(jnp.bfloat16), log_sums


def reference(tokens, w_query, w_key, w_value, w_out, chosen):
    mixed_list = []
    sums_list = []
    for seq_index in range(SEQS):
        mixed_one, sums_one = attend_sequence(tokens[seq_index], w_query, w_key, w_value, w_out, chosen[seq_index])
        mixed_list.append(mixed_one)
        sums_list.append(sums_one)
    return jnp.stack(mixed_list), jnp.stack(sums_list)
```

```python
import functools

import jax
import jax.numpy as jnp
from jax import lax
from jax.experimental import pallas as pl
from jax.experimental.pallas import tpu as pltpu
from jax.sharding import Mesh
from jax.sharding import PartitionSpec as P

HEAD_DIM = 64
BLOCK = 64
NZ, NY = 8, 4
CHUNKS = 2
GROUPS = ((0,), (1, 7), (2, 6), (3, 5), (4,))


def project_body(tok_ref, wk_ref, wv_ref, out_ref):
    width = wk_ref.shape[1]
    rows = tok_ref.shape[0]
    tok = tok_ref[...]
    keys = jnp.dot(tok, wk_ref[...], preferred_element_type=jnp.float32)
    vals = jnp.dot(tok, wv_ref[...], preferred_element_type=jnp.float32)
    out_ref[:, :, :width] = keys.astype(jnp.bfloat16).reshape(rows // BLOCK, BLOCK, width)
    out_ref[:, :, width:] = vals.astype(jnp.bfloat16).reshape(rows // BLOCK, BLOCK, width)


def project(tokens, w_key, w_value, chunk, width):
    rows, depth = tokens.shape
    tile = 128
    return pl.pallas_call(
        project_body,
        grid=(rows // tile,),
        in_specs=[
            pl.BlockSpec((tile, depth), lambda i: (i, 0)),
            pl.BlockSpec((depth, width), lambda i: (0, chunk)),
            pl.BlockSpec((depth, width), lambda i: (0, chunk)),
        ],
        out_specs=pl.BlockSpec((tile // BLOCK, BLOCK, 2 * width), lambda i: (i, 0, 0)),
        out_shape=jax.ShapeDtypeStruct((rows // BLOCK, BLOCK, 2 * width), jnp.bfloat16),
        name="project",
    )(tokens, w_key, w_value)


def pick_body(idx_ref, *refs, group):
    count = len(group)
    rows, outs, sems = refs[:count], refs[count : count + 3], refs[-1]
    copies = []
    for o in range(3):
        for n, r in enumerate(group):
            for e in range(2):
                copies.append(
                    pltpu.make_async_copy(
                        rows[n].at[idx_ref[(o * NZ + r) * 2 + e]],
                        outs[o].at[2 * n + e],
                        sems.at[len(copies)],
                    )
                )
    for copy in copies:
        copy.start()
    for copy in copies:
        copy.wait()


def pick(idx, rows, group):
    _, block, width = rows[0].shape
    shape = jax.ShapeDtypeStruct((2 * len(group), block, width), jnp.bfloat16)
    return pl.pallas_call(
        functools.partial(pick_body, group=group),
        in_specs=[pl.BlockSpec(memory_space=pltpu.SMEM)] + [pl.BlockSpec(memory_space=pl.ANY)] * len(rows),
        out_specs=[pl.BlockSpec(memory_space=pl.ANY)] * 3,
        out_shape=[shape] * 3,
        scratch_shapes=[pltpu.SemaphoreType.DMA((6 * len(group),))],
        name="pick",
    )(idx, *rows)


def attend_body(slot_ref, q_ref, *refs, width, picks):
    rows, got = refs[:NZ], refs[NZ : NZ + 3 * len(GROUPS)]
    att_ref, lse_ref, pool, sems = refs[NZ + 3 * len(GROUPS) :]
    copies = []
    for r in range(NZ):
        copies.append((rows[r], pool.at[pl.ds(8 * r, 8)]))
    for g, group in enumerate(GROUPS):
        for o in range(3):
            for n, r in enumerate(group):
                copies.append((got[3 * g + o].at[pl.ds(2 * n, 2)], pool.at[pl.ds(8 * NZ + (o * NZ + r) * 2, 2)]))
    copies = [pltpu.make_async_copy(a, b, sems.at[i]) for i, (a, b) in enumerate(copies)]
    for copy in copies:
        copy.start()
    for copy in copies:
        copy.wait()

    heads = width // HEAD_DIM
    span = heads * BLOCK
    neg = -jnp.inf
    lane_head = lax.broadcasted_iota(jnp.int32, (BLOCK, width), 1) // HEAD_DIM
    q_pos = lax.broadcasted_iota(jnp.int32, (span, 4 * BLOCK), 0) % BLOCK
    k_pos = lax.broadcasted_iota(jnp.int32, (span, 4 * BLOCK), 1)
    causal = (k_pos >= BLOCK) | (k_pos <= q_pos)
    slot_lane = lax.broadcasted_iota(jnp.int32, (1, 4 * BLOCK), 1) // BLOCK
    parts = picks // 4

    def one(b, carry):
        q = q_ref[pl.ds(pl.multiple_of(b * BLOCK, BLOCK), BLOCK), :]
        zero = jnp.zeros_like(q)
        q_bd = jnp.concatenate([jnp.where(lane_head == h, q, zero) for h in range(heads)], axis=0)
        slots = [slot_ref[b * picks + i] for i in range(picks)]
        safe = [jnp.maximum(s, 0) for s in slots]
        scores = []
        for t in range(parts):
            keys = jnp.concatenate([pool[safe[4 * t + i], :, :width] for i in range(4)], axis=0)
            s = lax.dot_general(q_bd, keys, (((1,), (1,)), ((), ())), preferred_element_type=jnp.float32)
            bias = jnp.zeros((1, 4 * BLOCK), jnp.float32)
            for i in range(4):
                bias = jnp.where((slot_lane == i) & (slots[4 * t + i] < 0), neg, bias)
            s = s + bias
            if t == 0:
                s = jnp.where(causal, s, neg)
            scores.append(s)
        top = functools.reduce(jnp.maximum, scores)
        row_max = jnp.max(top, axis=1, keepdims=True)
        total = None
        out = None
        for t in range(parts):
            e = jnp.exp(scores[t] - row_max)
            total = e if total is None else total + e
            vals = jnp.concatenate([pool[safe[4 * t + i], :, width:] for i in range(4)], axis=0)
            o = jnp.dot(e.astype(jnp.bfloat16), vals, preferred_element_type=jnp.float32)
            out = o if out is None else out + o
        row_sum = jnp.sum(total, axis=1, keepdims=True)
        out = out * (1.0 / row_sum)
        att = jnp.zeros((BLOCK, width), jnp.float32)
        for h in range(heads):
            att = jnp.where(lane_head == h, out[h * BLOCK : (h + 1) * BLOCK, :], att)
        att_ref[pl.ds(pl.multiple_of(b * BLOCK, BLOCK), BLOCK), :] = att.astype(jnp.bfloat16)
        lse = row_max + jnp.log(row_sum)
        lse_ref[pl.ds(b, 1), :] = jnp.broadcast_to(lse, (span, 128)).T[0:1, :]
        return carry

    lax.fori_loop(0, q_ref.shape[0] // BLOCK, one, 0)


def attend(slots, queries, rows, got, picks, width):
    tok = queries.shape[0]
    blocks = tok // BLOCK
    heads = width // HEAD_DIM
    return pl.pallas_call(
        functools.partial(attend_body, width=width, picks=picks),
        in_specs=[pl.BlockSpec(memory_space=pltpu.SMEM), pl.BlockSpec(memory_space=pltpu.VMEM)]
        + [pl.BlockSpec(memory_space=pl.ANY)] * (len(rows) + len(got)),
        out_specs=[pl.BlockSpec(memory_space=pltpu.VMEM), pl.BlockSpec(memory_space=pltpu.VMEM)],
        out_shape=[
            jax.ShapeDtypeStruct((tok, width), jnp.bfloat16),
            jax.ShapeDtypeStruct((blocks, heads * BLOCK), jnp.float32),
        ],
        scratch_shapes=[
            pltpu.VMEM((8 * NZ + 6 * NZ, BLOCK, 2 * width), jnp.bfloat16),
            pltpu.SemaphoreType.DMA((4 * NZ,)),
        ],
        compiler_params=pltpu.CompilerParams(vmem_limit_bytes=48 * 1024 * 1024),
        name="attend",
    )(slots, queries, *rows, *got)


def on_device(tokens, w_query, w_key, w_value, w_out, chosen):
    inputs = tokens[0]
    listed = chosen[0]
    tok_rows = inputs.shape[0]
    width = w_query.shape[1] // CHUNKS
    span_blocks = tok_rows // BLOCK
    query_count, picks = listed.shape
    my_z = lax.axis_index("z")
    my_y = lax.axis_index("y")
    my_t = lax.axis_index("tp")

    flat = listed.reshape(-1)
    valid = flat >= 0
    owner = jnp.where(valid, flat // span_blocks, -1)
    sources = jnp.arange(NZ * NY, dtype=jnp.int32)
    from_source = owner[None, :] == sources[:, None]
    least = jnp.min(jnp.where(from_source, flat[None, :], 1 << 20), axis=1)
    most = jnp.max(jnp.where(from_source, flat[None, :], -1), axis=1)
    most = jnp.maximum(most, 0)
    least = jnp.minimum(least, most)
    wanted = jnp.stack([least % span_blocks, most % span_blocks], axis=1).reshape(NZ, NY, 2)
    asked = []
    for o in (1, 2, 3):
        mine = lax.dynamic_index_in_dim(wanted, (my_y - o) % NY, axis=1, keepdims=False)
        asked.append(lax.ppermute(mine, "y", [((i + o) % NY, i) for i in range(NY)]))
    asked = jnp.stack(asked)
    back = (my_z - jnp.arange(NZ, dtype=jnp.int32)) % NZ
    pick_idx = asked[:, back, :].reshape(-1)

    src_z = owner // NY
    src_y = owner % NY
    step = (my_z - src_z) % NZ
    off = (my_y - src_y) % NY
    second = jnp.any((owner[:, None] == owner[None, :]) & (flat[None, :] < flat[:, None]), axis=1)
    slots = jnp.where(
        off == 0,
        step * 8 + flat % span_blocks,
        8 * NZ + ((off - 1) * NZ + step) * 2 + second.astype(jnp.int32),
    )
    slots = jnp.where(valid, slots, -1)

    up = [(i, (i + 1) % NZ) for i in range(NZ)]
    down = [(i, (i - 1) % NZ) for i in range(NZ)]
    chunk_rows = [project(inputs, w_key, w_value, c, width) for c in range(CHUNKS)]
    rows = [{0: chunk_rows[c]} for c in range(CHUNKS)]
    got = [[] for _ in range(CHUNKS)]
    for g, group in enumerate(GROUPS):
        for c in range(CHUNKS):
            if g > 0:
                for r in group:
                    if r <= NZ // 2:
                        rows[c][r] = lax.ppermute(rows[c][r - 1], "z", up)
                    else:
                        rows[c][r] = lax.ppermute(rows[c][(r + 1) % NZ], "z", down)
            sends = pick(pick_idx, [rows[c][r] for r in group], group)
            for o in range(3):
                got[c].append(lax.ppermute(sends[o], "y", [(i, (i + o + 1) % NY) for i in range(NY)]))

    queries = jnp.dot(inputs, w_query, preferred_element_type=jnp.float32).astype(jnp.bfloat16)
    queries = queries * jnp.bfloat16(HEAD_DIM**-0.5)
    attended, sums = [], []
    for c in range(CHUNKS):
        a, s = attend(
            slots, queries[:, c * width : (c + 1) * width], [rows[c][r] for r in range(NZ)], got[c], picks, width
        )
        attended.append(a)
        sums.append(s.reshape(query_count, width // HEAD_DIM, BLOCK))
    attended = jnp.concatenate(attended, axis=1)
    log_sums = jnp.concatenate(sums, axis=1).transpose(1, 0, 2).reshape(-1, tok_rows)

    half = tok_rows // 2
    theirs = lax.dynamic_slice_in_dim(attended, (1 - my_t) * half, half, axis=0)
    mine = lax.dynamic_slice_in_dim(attended, my_t * half, half, axis=0)
    away = jnp.dot(theirs, w_out, preferred_element_type=jnp.float32).astype(jnp.bfloat16)
    came = lax.ppermute(away, "tp", [(0, 1), (1, 0)])
    here = jnp.dot(mine, w_out, preferred_element_type=jnp.float32).astype(jnp.bfloat16)
    mixed = (here.astype(jnp.float32) + came.astype(jnp.float32)).astype(jnp.bfloat16)
    return (mixed[None], log_sums[None])


def solution(mesh):
    devices = mesh.devices
    split = Mesh(devices.reshape(devices.shape[0], NZ, NY, devices.shape[2]), ("dp", "z", "y", "tp"))
    return jax.shard_map(
        on_device,
        mesh=split,
        in_specs=(
            P("dp", ("z", "y"), None),
            P(None, "tp"),
            P(None, "tp"),
            P(None, "tp"),
            P("tp", None),
            P("dp", ("z", "y"), None),
        ),
        out_specs=(P("dp", ("z", "y", "tp"), None), P("dp", "tp", ("z", "y"))),
        check_vma=False,
    )
```

```python
import functools

import jax
import jax.numpy as jnp
from jax import lax
from jax.experimental import pallas as pl
from jax.experimental.pallas import tpu as pltpu
from jax.sharding import Mesh
from jax.sharding import PartitionSpec as P


HEAD_DIM = 64
BLOCK = 64
NZ, NY = 8, 4
CHUNKS = 2
GROUPS = ((0,), (1, 7), (2, 6), (3, 5), (4,))


def project_body(tok_ref, wk_ref, wv_ref, *out_refs):
    rows = tok_ref.shape[0]
    width = wk_ref.shape[1] // CHUNKS
    tok = tok_ref[...]
    keys = jnp.dot(tok, wk_ref[...], preferred_element_type=jnp.float32).astype(jnp.bfloat16)
    vals = jnp.dot(tok, wv_ref[...], preferred_element_type=jnp.float32).astype(jnp.bfloat16)
    for c, out_ref in enumerate(out_refs):
        cut = slice(c * width, (c + 1) * width)
        out_ref[:, :, :width] = keys[:, cut].reshape(rows // BLOCK, BLOCK, width)
        out_ref[:, :, width:] = vals[:, cut].reshape(rows // BLOCK, BLOCK, width)


def project(tokens, w_key, w_value):
    rows, depth = tokens.shape
    cols = w_key.shape[1]
    tile = 128
    each = 2 * cols // CHUNKS
    return pl.pallas_call(
        project_body,
        grid=(rows // tile,),
        in_specs=[
            pl.BlockSpec((tile, depth), lambda i: (i, 0)),
            pl.BlockSpec((depth, cols), lambda i: (0, 0)),
            pl.BlockSpec((depth, cols), lambda i: (0, 0)),
        ],
        out_specs=[pl.BlockSpec((tile // BLOCK, BLOCK, each), lambda i: (i, 0, 0))] * CHUNKS,
        out_shape=[jax.ShapeDtypeStruct((rows // BLOCK, BLOCK, each), jnp.bfloat16)] * CHUNKS,
        name="project",
    )(tokens, w_key, w_value)


def pick_body(idx_ref, *refs, group):
    count = len(group)
    rows, outs, sems = refs[:count], refs[count : count + 3], refs[-1]
    copies = []
    for o in range(3):
        for n, r in enumerate(group):
            for e in range(2):
                copies.append(
                    pltpu.make_async_copy(
                        rows[n].at[idx_ref[(o * NZ + r) * 2 + e]],
                        outs[o].at[2 * n + e],
                        sems.at[len(copies)],
                    )
                )
    for copy in copies:
        copy.start()
    for copy in copies:
        copy.wait()


def pick(idx, rows, group):
    _, block, width = rows[0].shape
    shape = jax.ShapeDtypeStruct((2 * len(group), block, width), jnp.bfloat16)
    return pl.pallas_call(
        functools.partial(pick_body, group=group),
        in_specs=[pl.BlockSpec(memory_space=pltpu.SMEM)] + [pl.BlockSpec(memory_space=pl.ANY)] * len(rows),
        out_specs=[pl.BlockSpec(memory_space=pltpu.VMEM)] * 3,
        out_shape=[shape] * 3,
        scratch_shapes=[pltpu.SemaphoreType.DMA((6 * len(group),))],
        name="pick",
    )(idx, *rows)


def attend_body(slot_ref, q_ref, *refs, width, picks):
    rows, got = refs[:NZ], refs[NZ : NZ + 3 * len(GROUPS)]
    att_ref, lse_ref, pool, sems = refs[NZ + 3 * len(GROUPS) :]
    copies = []
    for r in range(NZ):
        copies.append((rows[r], pool.at[pl.ds(8 * r, 8)]))
    for g, group in enumerate(GROUPS):
        for o in range(3):
            for n, r in enumerate(group):
                copies.append((got[3 * g + o].at[pl.ds(2 * n, 2)], pool.at[pl.ds(8 * NZ + (o * NZ + r) * 2, 2)]))
    copies = [pltpu.make_async_copy(a, b, sems.at[i]) for i, (a, b) in enumerate(copies)]
    for copy in copies:
        copy.start()
    for copy in copies:
        copy.wait()

    heads = width // HEAD_DIM
    span = heads * BLOCK
    neg = -jnp.inf
    lane_head = lax.broadcasted_iota(jnp.int32, (BLOCK, width), 1) // HEAD_DIM
    q_pos = lax.broadcasted_iota(jnp.int32, (span, 4 * BLOCK), 0) % BLOCK
    k_pos = lax.broadcasted_iota(jnp.int32, (span, 4 * BLOCK), 1)
    causal = (k_pos >= BLOCK) | (k_pos <= q_pos)
    slot_lane = lax.broadcasted_iota(jnp.int32, (1, 4 * BLOCK), 1) // BLOCK
    parts = picks // 4

    def one(b, carry):
        q = q_ref[pl.ds(pl.multiple_of(b * BLOCK, BLOCK), BLOCK), :]
        zero = jnp.zeros_like(q)
        q_bd = jnp.concatenate([jnp.where(lane_head == h, q, zero) for h in range(heads)], axis=0)
        slots = [slot_ref[b * picks + i] for i in range(picks)]
        safe = [jnp.maximum(s, 0) for s in slots]
        scores = []
        for t in range(parts):
            keys = jnp.concatenate([pool[safe[4 * t + i], :, :width] for i in range(4)], axis=0)
            s = lax.dot_general(q_bd, keys, (((1,), (1,)), ((), ())), preferred_element_type=jnp.float32)
            bias = jnp.zeros((1, 4 * BLOCK), jnp.float32)
            for i in range(4):
                bias = jnp.where((slot_lane == i) & (slots[4 * t + i] < 0), neg, bias)
            s = s + bias
            if t == 0:
                s = jnp.where(causal, s, neg)
            scores.append(s)
        top = functools.reduce(jnp.maximum, scores)
        row_max = jnp.max(top, axis=1, keepdims=True)
        total = None
        out = None
        for t in range(parts):
            e = jnp.exp(scores[t] - row_max)
            total = e if total is None else total + e
            vals = jnp.concatenate([pool[safe[4 * t + i], :, width:] for i in range(4)], axis=0)
            o = jnp.dot(e.astype(jnp.bfloat16), vals, preferred_element_type=jnp.float32)
            out = o if out is None else out + o
        row_sum = jnp.sum(total, axis=1, keepdims=True)
        out = out * (1.0 / row_sum)
        att = jnp.zeros((BLOCK, width), jnp.float32)
        for h in range(heads):
            att = jnp.where(lane_head == h, out[h * BLOCK : (h + 1) * BLOCK, :], att)
        att_ref[pl.ds(pl.multiple_of(b * BLOCK, BLOCK), BLOCK), :] = att.astype(jnp.bfloat16)
        lse = row_max + jnp.log(row_sum)
        lse_ref[pl.ds(b, 1), :] = jnp.broadcast_to(lse, (span, 128)).T[0:1, :]
        return carry

    lax.fori_loop(0, q_ref.shape[0] // BLOCK, one, 0)


def attend(slots, queries, rows, got, picks, width):
    tok = queries.shape[0]
    blocks = tok // BLOCK
    heads = width // HEAD_DIM
    return pl.pallas_call(
        functools.partial(attend_body, width=width, picks=picks),
        in_specs=[pl.BlockSpec(memory_space=pltpu.SMEM), pl.BlockSpec(memory_space=pltpu.VMEM)]
        + [pl.BlockSpec(memory_space=pl.ANY)] * (len(rows) + len(got)),
        out_specs=[pl.BlockSpec(memory_space=pltpu.VMEM), pl.BlockSpec(memory_space=pltpu.VMEM)],
        out_shape=[
            jax.ShapeDtypeStruct((tok, width), jnp.bfloat16),
            jax.ShapeDtypeStruct((blocks, heads * BLOCK), jnp.float32),
        ],
        scratch_shapes=[
            pltpu.VMEM((8 * NZ + 6 * NZ, BLOCK, 2 * width), jnp.bfloat16),
            pltpu.SemaphoreType.DMA((4 * NZ,)),
        ],
        compiler_params=pltpu.CompilerParams(vmem_limit_bytes=48 * 1024 * 1024),
        name="attend",
    )(slots, queries, *rows, *got)


def on_device(tokens, w_query, w_key, w_value, w_out, chosen):
    inputs = tokens[0]
    listed = chosen[0]
    tok_rows = inputs.shape[0]
    width = w_query.shape[1] // CHUNKS
    span_blocks = tok_rows // BLOCK
    query_count, picks = listed.shape
    my_z = lax.axis_index("z")
    my_y = lax.axis_index("y")
    my_t = lax.axis_index("tp")

    flat = listed.reshape(-1)
    valid = flat >= 0
    owner = jnp.where(valid, flat // span_blocks, -1)
    sources = jnp.arange(NZ * NY, dtype=jnp.int32)
    from_source = owner[None, :] == sources[:, None]
    least = jnp.min(jnp.where(from_source, flat[None, :], 1 << 20), axis=1)
    most = jnp.max(jnp.where(from_source, flat[None, :], -1), axis=1)
    most = jnp.maximum(most, 0)
    least = jnp.minimum(least, most)
    wanted = jnp.stack([least % span_blocks, most % span_blocks], axis=1).reshape(NZ, NY, 2)
    mine = [lax.dynamic_index_in_dim(wanted, (my_y - o) % NY, axis=1, keepdims=False) for o in (1, 2, 3)]
    inputs, *mine = lax.optimization_barrier((inputs, *mine))
    asked = [lax.ppermute(m, "y", [((i + o) % NY, i) for i in range(NY)]) for o, m in zip((1, 2, 3), mine)]
    asked = jnp.stack(asked)
    back = (my_z - jnp.arange(NZ, dtype=jnp.int32)) % NZ
    pick_idx = asked[:, back, :].reshape(-1)

    src_z = owner // NY
    src_y = owner % NY
    step = (my_z - src_z) % NZ
    off = (my_y - src_y) % NY
    second = jnp.any((owner[:, None] == owner[None, :]) & (flat[None, :] < flat[:, None]), axis=1)
    slots = jnp.where(
        off == 0,
        step * 8 + flat % span_blocks,
        8 * NZ + ((off - 1) * NZ + step) * 2 + second.astype(jnp.int32),
    )
    slots = jnp.where(valid, slots, -1)

    up = [(i, (i + 1) % NZ) for i in range(NZ)]
    down = [(i, (i - 1) % NZ) for i in range(NZ)]
    rows = [{0: first} for first in project(inputs, w_key, w_value)]
    got = [[] for _ in range(CHUNKS)]
    for g, group in enumerate(GROUPS):
        for c in range(CHUNKS):
            here = [rows[c][r] for r in group]
            if g + 1 < len(GROUPS):
                for r in GROUPS[g + 1]:
                    if r <= NZ // 2:
                        rows[c][r] = lax.ppermute(rows[c][r - 1], "z", up)
                    else:
                        rows[c][r] = lax.ppermute(rows[c][(r + 1) % NZ], "z", down)
            sends = pick(pick_idx, here, group)
            for o in range(3):
                got[c].append(lax.ppermute(sends[o], "y", [(i, (i + o + 1) % NY) for i in range(NY)]))

    queries = jnp.dot(inputs, w_query, preferred_element_type=jnp.float32).astype(jnp.bfloat16)
    queries = queries * jnp.bfloat16(HEAD_DIM**-0.5)
    attended, sums = [], []
    for c in range(CHUNKS):
        a, s = attend(
            slots, queries[:, c * width : (c + 1) * width], [rows[c][r] for r in range(NZ)], got[c], picks, width
        )
        attended.append(a)
        sums.append(s.reshape(query_count, width // HEAD_DIM, BLOCK))
    attended = jnp.concatenate(attended, axis=1)
    log_sums = jnp.concatenate(sums, axis=1).transpose(1, 0, 2).reshape(-1, tok_rows)

    half = tok_rows // 2
    theirs = lax.dynamic_slice_in_dim(attended, (1 - my_t) * half, half, axis=0)
    mine = lax.dynamic_slice_in_dim(attended, my_t * half, half, axis=0)
    away = jnp.dot(theirs, w_out, preferred_element_type=jnp.float32).astype(jnp.bfloat16)
    came = lax.ppermute(away, "tp", [(0, 1), (1, 0)])
    here = jnp.dot(mine, w_out, preferred_element_type=jnp.float32).astype(jnp.bfloat16)
    mixed = (here.astype(jnp.float32) + came.astype(jnp.float32)).astype(jnp.bfloat16)
    return (mixed[None], log_sums[None])


def solution(mesh):
    devices = mesh.devices
    split = Mesh(devices.reshape(devices.shape[0], NZ, NY, devices.shape[2]), ("dp", "z", "y", "tp"))
    return jax.shard_map(
        on_device,
        mesh=split,
        in_specs=(
            P("dp", ("z", "y"), None),
            P(None, "tp"),
            P(None, "tp"),
            P(None, "tp"),
            P("tp", None),
            P("dp", ("z", "y"), None),
        ),
        out_specs=(P("dp", ("z", "y", "tp"), None), P("dp", "tp", ("z", "y"))),
        check_vma=False,
    )
```

```python
import functools

import jax
import jax.numpy as jnp
from jax import lax
from jax.experimental import pallas as pl
from jax.experimental.pallas import tpu as pltpu
from jax.sharding import Mesh
from jax.sharding import PartitionSpec as P


HEAD_DIM = 64
BLOCK = 64
NZ, NY = 8, 4
CHUNKS = 2
EVENTS = (
    ((0, 0), (1, 0)),
    ((0, 1), (0, 7)),
    ((1, 1), (1, 7)),
    ((0, 2), (0, 6)),
    ((1, 2), (1, 6)),
    ((0, 3), (0, 5)),
    ((1, 3), (1, 5)),
    ((0, 4), (1, 4)),
)
FOLLOW = (
    ((0, 1), (0, 7), (1, 1), (1, 7)),
    ((0, 2), (0, 6)),
    ((1, 2), (1, 6)),
    ((0, 3), (0, 5)),
    ((1, 3), (1, 5)),
    ((0, 4),),
    ((1, 4),),
    (),
)


def project_body(tok_ref, wk_ref, wv_ref, *refs):
    out_refs, (keys, vals) = refs[:CHUNKS], refs[CHUNKS:]
    rows = tok_ref.shape[0]
    width = wk_ref.shape[1] // CHUNKS
    step = pl.program_id(0)
    tok = tok_ref[...]
    k = jnp.dot(tok, wk_ref[...], preferred_element_type=jnp.float32)
    v = jnp.dot(tok, wv_ref[...], preferred_element_type=jnp.float32)

    @pl.when(step == 0)
    def _():
        keys[...] = k
        vals[...] = v

    @pl.when((step > 0) & (step < pl.num_programs(0) - 1))
    def _():
        keys[...] += k
        vals[...] += v

    @pl.when(step == pl.num_programs(0) - 1)
    def _():
        all_k = (keys[...] + k).astype(jnp.bfloat16)
        all_v = (vals[...] + v).astype(jnp.bfloat16)
        for c, out_ref in enumerate(out_refs):
            cut = slice(c * width, (c + 1) * width)
            out_ref[:, :, :width] = all_k[:, cut].reshape(rows // BLOCK, BLOCK, width)
            out_ref[:, :, width:] = all_v[:, cut].reshape(rows // BLOCK, BLOCK, width)


def project(tokens, w_key, w_value):
    rows, depth = tokens.shape
    cols = w_key.shape[1]
    tile = 512
    each = 2 * cols // CHUNKS
    return pl.pallas_call(
        project_body,
        grid=(depth // tile,),
        in_specs=[
            pl.BlockSpec((rows, tile), lambda i: (0, i)),
            pl.BlockSpec((tile, cols), lambda i: (i, 0)),
            pl.BlockSpec((tile, cols), lambda i: (i, 0)),
        ],
        out_specs=[pl.BlockSpec((rows // BLOCK, BLOCK, each), lambda i: (0, 0, 0))] * CHUNKS,
        out_shape=[jax.ShapeDtypeStruct((rows // BLOCK, BLOCK, each), jnp.bfloat16)] * CHUNKS,
        scratch_shapes=[pltpu.VMEM((rows, cols), jnp.float32)] * 2,
        name="project",
    )(tokens, w_key, w_value)


def pick_body(idx_ref, *refs, steps):
    count = len(steps)
    rows, outs, sems = refs[:count], refs[count : count + 3], refs[-1]
    copies = []
    for o in range(3):
        for n, r in enumerate(steps):
            for e in range(2):
                copies.append(
                    pltpu.make_async_copy(
                        rows[n].at[idx_ref[(o * NZ + r) * 2 + e]],
                        outs[o].at[2 * n + e],
                        sems.at[len(copies)],
                    )
                )
    for copy in copies:
        copy.start()
    for copy in copies:
        copy.wait()


def pick(idx, rows, steps):
    _, block, width = rows[0].shape
    shape = jax.ShapeDtypeStruct((2 * len(steps), block, width), jnp.bfloat16)
    return pl.pallas_call(
        functools.partial(pick_body, steps=steps),
        in_specs=[pl.BlockSpec(memory_space=pltpu.SMEM)] + [pl.BlockSpec(memory_space=pl.ANY)] * len(rows),
        out_specs=[pl.BlockSpec(memory_space=pltpu.VMEM)] * 3,
        out_shape=[shape] * 3,
        scratch_shapes=[pltpu.SemaphoreType.DMA((6 * len(steps),))],
        name="pick",
    )(idx, *rows)


def attend_body(slot_ref, q_ref, *refs, width, picks, places):
    rows, got = refs[:NZ], refs[NZ : NZ + 3 * len(places)]
    att_ref, lse_ref, pool, sems = refs[NZ + 3 * len(places) :]
    copies = []
    for r in range(NZ):
        copies.append((rows[r], pool.at[pl.ds(8 * r, 8)]))
    for e, place in enumerate(places):
        for o in range(3):
            for n, r in place:
                copies.append((got[3 * e + o].at[pl.ds(2 * n, 2)], pool.at[pl.ds(8 * NZ + (o * NZ + r) * 2, 2)]))
    copies = [pltpu.make_async_copy(a, b, sems.at[i]) for i, (a, b) in enumerate(copies)]
    for copy in copies:
        copy.start()
    for copy in copies:
        copy.wait()

    heads = width // HEAD_DIM
    span = heads * BLOCK
    neg = -jnp.inf
    lane_head = lax.broadcasted_iota(jnp.int32, (BLOCK, width), 1) // HEAD_DIM
    q_pos = lax.broadcasted_iota(jnp.int32, (span, 4 * BLOCK), 0) % BLOCK
    k_pos = lax.broadcasted_iota(jnp.int32, (span, 4 * BLOCK), 1)
    causal = (k_pos >= BLOCK) | (k_pos <= q_pos)
    slot_lane = lax.broadcasted_iota(jnp.int32, (1, 4 * BLOCK), 1) // BLOCK
    parts = picks // 4

    def one(b, carry):
        q = q_ref[pl.ds(pl.multiple_of(b * BLOCK, BLOCK), BLOCK), :]
        zero = jnp.zeros_like(q)
        q_bd = jnp.concatenate([jnp.where(lane_head == h, q, zero) for h in range(heads)], axis=0)
        slots = [slot_ref[b * picks + i] for i in range(picks)]
        safe = [jnp.maximum(s, 0) for s in slots]
        scores = []
        for t in range(parts):
            keys = jnp.concatenate([pool[safe[4 * t + i], :, :width] for i in range(4)], axis=0)
            s = lax.dot_general(q_bd, keys, (((1,), (1,)), ((), ())), preferred_element_type=jnp.float32)
            bias = jnp.zeros((1, 4 * BLOCK), jnp.float32)
            for i in range(4):
                bias = jnp.where((slot_lane == i) & (slots[4 * t + i] < 0), neg, bias)
            s = s + bias
            if t == 0:
                s = jnp.where(causal, s, neg)
            scores.append(s)
        top = functools.reduce(jnp.maximum, scores)
        row_max = jnp.max(top, axis=1, keepdims=True)
        total = None
        out = None
        for t in range(parts):
            e = jnp.exp(scores[t] - row_max)
            total = e if total is None else total + e
            vals = jnp.concatenate([pool[safe[4 * t + i], :, width:] for i in range(4)], axis=0)
            o = jnp.dot(e.astype(jnp.bfloat16), vals, preferred_element_type=jnp.float32)
            out = o if out is None else out + o
        row_sum = jnp.sum(total, axis=1, keepdims=True)
        out = out * (1.0 / row_sum)
        att = jnp.zeros((BLOCK, width), jnp.float32)
        for h in range(heads):
            att = jnp.where(lane_head == h, out[h * BLOCK : (h + 1) * BLOCK, :], att)
        att_ref[pl.ds(pl.multiple_of(b * BLOCK, BLOCK), BLOCK), :] = att.astype(jnp.bfloat16)
        lse = row_max + jnp.log(row_sum)
        lse_ref[pl.ds(b, 1), :] = jnp.broadcast_to(lse, (span, 128)).T[0:1, :]
        return carry

    lax.fori_loop(0, q_ref.shape[0] // BLOCK, one, 0)


def attend(slots, queries, rows, got, places, picks, width):
    tok = queries.shape[0]
    blocks = tok // BLOCK
    heads = width // HEAD_DIM
    return pl.pallas_call(
        functools.partial(attend_body, width=width, picks=picks, places=places),
        in_specs=[pl.BlockSpec(memory_space=pltpu.SMEM), pl.BlockSpec(memory_space=pltpu.VMEM)]
        + [pl.BlockSpec(memory_space=pl.ANY)] * (len(rows) + len(got)),
        out_specs=[pl.BlockSpec(memory_space=pltpu.VMEM), pl.BlockSpec(memory_space=pltpu.VMEM)],
        out_shape=[
            jax.ShapeDtypeStruct((tok, width), jnp.bfloat16),
            jax.ShapeDtypeStruct((blocks, heads * BLOCK), jnp.float32),
        ],
        scratch_shapes=[
            pltpu.VMEM((8 * NZ + 6 * NZ, BLOCK, 2 * width), jnp.bfloat16),
            pltpu.SemaphoreType.DMA((4 * NZ,)),
        ],
        compiler_params=pltpu.CompilerParams(vmem_limit_bytes=48 * 1024 * 1024),
        name="attend",
    )(slots, queries, *rows, *got)


def on_device(tokens, w_query, w_key, w_value, w_out, chosen):
    inputs = tokens[0]
    listed = chosen[0]
    tok_rows = inputs.shape[0]
    width = w_query.shape[1] // CHUNKS
    span_blocks = tok_rows // BLOCK
    query_count, picks = listed.shape
    my_z = lax.axis_index("z")
    my_y = lax.axis_index("y")
    my_t = lax.axis_index("tp")

    flat = listed.reshape(-1)
    valid = flat >= 0
    owner = jnp.where(valid, flat // span_blocks, -1)
    sources = jnp.arange(NZ * NY, dtype=jnp.int32)
    from_source = owner[None, :] == sources[:, None]
    least = jnp.min(jnp.where(from_source, flat[None, :], 1 << 20), axis=1)
    most = jnp.max(jnp.where(from_source, flat[None, :], -1), axis=1)
    most = jnp.maximum(most, 0)
    least = jnp.minimum(least, most)
    wanted = jnp.stack([least % span_blocks, most % span_blocks], axis=1).reshape(NZ, NY, 2)
    wanted = jnp.moveaxis(wanted, 1, 0)
    inputs, wanted = lax.optimization_barrier((inputs, wanted))
    asked = lax.all_to_all(wanted, "y", 0, 0, tiled=True)
    asked = asked[(my_y + jnp.arange(1, NY, dtype=jnp.int32)) % NY]
    back = (my_z - jnp.arange(NZ, dtype=jnp.int32)) % NZ
    pick_idx = asked[:, back, :].reshape(-1)

    src_z = owner // NY
    src_y = owner % NY
    step = (my_z - src_z) % NZ
    off = (my_y - src_y) % NY
    second = jnp.any((owner[:, None] == owner[None, :]) & (flat[None, :] < flat[:, None]), axis=1)
    slots = jnp.where(
        off == 0,
        step * 8 + flat % span_blocks,
        8 * NZ + ((off - 1) * NZ + step) * 2 + second.astype(jnp.int32),
    )
    slots = jnp.where(valid, slots, -1)

    up = [(i, (i + 1) % NZ) for i in range(NZ)]
    down = [(i, (i - 1) % NZ) for i in range(NZ)]
    rows = [{0: first} for first in project(inputs, w_key, w_value)]
    got = [[] for _ in range(CHUNKS)]
    places = [[] for _ in range(CHUNKS)]
    for e, event in enumerate(EVENTS):
        for c, r in FOLLOW[e]:
            if r < 4 or (r == 4 and c == 0):
                rows[c][r] = lax.ppermute(rows[c][r - 1], "z", up)
            else:
                rows[c][r] = lax.ppermute(rows[c][(r + 1) % NZ], "z", down)
        sends = pick(pick_idx, [rows[c][r] for c, r in event], tuple(r for _, r in event))
        sent = []
        for o in range(3):
            sent.append(lax.ppermute(sends[o], "y", [(i, (i + o + 1) % NY) for i in range(NY)]))
        for c in range(CHUNKS):
            place = tuple((n, r) for n, (ec, r) in enumerate(event) if ec == c)
            if place:
                got[c].extend(sent)
                places[c].append(place)

    queries = jnp.dot(inputs, w_query, preferred_element_type=jnp.float32).astype(jnp.bfloat16)
    queries = queries * jnp.bfloat16(HEAD_DIM**-0.5)
    attended, sums = [], []
    for c in range(CHUNKS):
        a, s = attend(
            slots,
            queries[:, c * width : (c + 1) * width],
            [rows[c][r] for r in range(NZ)],
            got[c],
            tuple(places[c]),
            picks,
            width,
        )
        attended.append(a)
        sums.append(s.reshape(query_count, width // HEAD_DIM, BLOCK))
    attended = jnp.concatenate(attended, axis=1)
    log_sums = jnp.concatenate(sums, axis=1).transpose(1, 0, 2).reshape(-1, tok_rows)

    half = tok_rows // 2
    theirs = lax.dynamic_slice_in_dim(attended, (1 - my_t) * half, half, axis=0)
    mine = lax.dynamic_slice_in_dim(attended, my_t * half, half, axis=0)
    away = jnp.dot(theirs, w_out, preferred_element_type=jnp.float32).astype(jnp.bfloat16)
    came = lax.ppermute(away, "tp", [(0, 1), (1, 0)])
    here = jnp.dot(mine, w_out, preferred_element_type=jnp.float32).astype(jnp.bfloat16)
    mixed = (here.astype(jnp.float32) + came.astype(jnp.float32)).astype(jnp.bfloat16)
    return (mixed[None], log_sums[None])


def solution(mesh):
    devices = mesh.devices
    split = Mesh(devices.reshape(devices.shape[0], NZ, NY, devices.shape[2]), ("dp", "z", "y", "tp"))
    return jax.shard_map(
        on_device,
        mesh=split,
        in_specs=(
            P("dp", ("z", "y"), None),
            P(None, "tp"),
            P(None, "tp"),
            P(None, "tp"),
            P("tp", None),
            P("dp", ("z", "y"), None),
        ),
        out_specs=(P("dp", ("z", "y", "tp"), None), P("dp", "tp", ("z", "y"))),
        check_vma=False,
    )
```
